32 devices in a mesh: row: 8 (over z, x), col: 4 (over y, core).
Axes of the slice: x: 2, y: 2, z: 4, core: 2. Of those that a mesh axis runs over, the one named last changes fastest.
Arguments:
- tokens: bfloat16 [1024, 4096], P('row'), may hold values from -6 to 6
- w_value: bfloat16 [2304, 4096], P('col'), may hold values from -0.09375 to 0.09375
- w_gate_one: bfloat16 [2304, 4096], P('col'), may hold values from -0.09375 to 0.09375
- w_gate_two: bfloat16 [2304, 4096], P('col'), may hold values from -0.09375 to 0.09375
- short_taps: float32 [3, 3, 2304], P(None, None, 'col'), may hold values from -3.5 to 3.5
- filter_in: float32 [33, 64], replicated, may hold values from -1 to 1
- filter_mid: float32 [64, 64], replicated, may hold values from -0.75 to 0.75
- filter_out: float32 [64, 2, 2, 2304], replicated, may hold values from -1 to 1
- decay_rate: float32 [2304], P('col'), may hold values from 0.5 to 9, as said below
- skip: float32 [2, 2304], P(None, 'col'), may hold values from -0.3 to 0.3
- w_out: bfloat16 [2304, 4096], P(None, 'col'), may hold values from -0.125 to 0.125
Outputs:
- mixed: bfloat16 [1024, 4096], P('row', 'col')
The draws below stay inside these ranges and needn't reach their ends.
Inputs may be any that keep to these rules, and one draw needn't show every extreme that they name: `decay_rate`: each channel's rate is positive; per unit of the relative position t.
All inputs are finite; a program needn't handle non-finite values.
Results may differ from the reference program's by a relative error of at most 0.007.
Values may be sent and summed in bfloat16 or wider, within the bound.
A program may use at most 64 MiB of HBM per device.

```python
import math
import jax
import jax.numpy as jnp
from jax import lax

D = 4096
HW = 2304
FILTER_HID = 64
BANDS = 16
EMB = 33
SEQ = 1024


def channel_rates(key, fast_share):
    key_slow, key_fast, key_pick = jax.random.split(jax.random.fold_in(key, 11), 3)
    slow_rates = jnp.exp(jax.random.uniform(key_slow, (HW,), jnp.float32, math.log(0.5), math.log(2.0)))
    fast_rates = jnp.exp(jax.random.uniform(key_fast, (HW,), jnp.float32, math.log(SEQ / 154.0), math.log(SEQ / 128.0)))
    chosen = jax.random.uniform(key_pick, (HW,), jnp.float32) < fast_share
    return jnp.where(chosen, fast_rates, slow_rates)


def draw_decay_rate(key, part):
    fast_share = 0.5
    return channel_rates(key, fast_share)


def draw_filter_out(key, part):
    fast_share = 0.5
    rates = channel_rates(key, fast_share)
    column_scale = jnp.sqrt(2.0 * rates / (1.0 - jnp.exp(-2.0 * rates)))
    noise = jax.random.truncated_normal(jax.random.fold_in(key, 23), -4.0, 4.0, (FILTER_HID, 2, 2, HW), jnp.float32)
    return noise * column_scale / math.sqrt(FILTER_HID * SEQ)


def steps_of(own_key, shape, cuts, least, largest):
    def one(position, blocks):
        heights = jax.random.uniform(jax.random.fold_in(jax.random.fold_in(own_key, 6), position), (blocks,), jnp.float32, least / len(cuts), largest / len(cuts))
        return jnp.repeat(jnp.exp(heights), shape[position] // blocks).reshape((-1,) + (1,) * (len(shape) - position - 1))

    loudness = one(*cuts[0])
    for cut in cuts[1:]:
        loudness = loudness * one(*cut)
    return loudness


def gaussian(own_key, extent, width, most, pieces=(), kind=jnp.bfloat16):
    array = jax.random.normal(own_key, extent, jnp.float32) * width
    if len(pieces) > 0:
        array = steps_of(own_key, extent, pieces, -0.22, 0.18) * array
    return jnp.clip(array, min=-most, max=most).astype(kind)


def setup_inputs(seed: int = 0) -> dict:
    splits = jax.random.split(jax.random.key(seed), 12)
    return {
        "tokens": gaussian(splits[0], (SEQ, D), 1.0, 6.0, ((0, 8),)),
        "w_value": gaussian(splits[1], (HW, D), D ** -0.5, 0.09375, ((0, 4),)),
        "w_gate_one": gaussian(splits[2], (HW, D), D ** -0.5, 0.09375, ((0, 4),)),
        "w_gate_two": gaussian(splits[3], (HW, D), D ** -0.5, 0.09375, ((0, 4),)),
        "short_taps": gaussian(splits[4], (3, 3, HW), 3 ** -0.5, 3.5, ((2, 4),), jnp.float32),
        "filter_in": jnp.clip(jax.random.uniform(splits[5], (EMB, FILTER_HID), jnp.float32, -1.0, 1.0), -1.0, 1.0),
        "filter_mid": jnp.clip(jax.random.uniform(splits[6], (FILTER_HID, FILTER_HID), jnp.float32, -0.75, 0.75), -0.75, 0.75),
        "filter_out": draw_filter_out(jax.random.fold_in(splits[11], 71), 0),
        "decay_rate": draw_decay_rate(jax.random.fold_in(splits[11], 71), 0),
        "skip": jnp.clip(jax.random.uniform(splits[9], (2, HW), jnp.float32, -0.3, 0.3) * steps_of(splits[9], (2, HW), ((1, 4),), -0.4, 0.0), -0.3, 0.3),
        "w_out": gaussian(splits[10], (HW, D), HW ** -0.5, 0.125, ((1, 4),)),
    }


HIGHEST = lax.Precision.HIGHEST


def filter_bank(filter_in, filter_mid, out_block, rate_block):
    positions = jnp.arange(SEQ, dtype=jnp.float32)
    relative = positions / (SEQ - 1)
    bands = jnp.linspace(1e-4, BANDS - 1, BANDS, dtype=jnp.float32)
    angles = (2 * math.pi / SEQ) * positions[:, None] * bands[None, :]
    feats = jnp.concatenate([relative[:, None], jnp.cos(angles), jnp.sin(angles)], axis=1)
    hidden = jnp.sin(jnp.dot(feats, filter_in, precision=HIGHEST))
    hidden = jnp.sin(jnp.dot(hidden, filter_mid, precision=HIGHEST))
    filter_taps = jnp.einsum('lh,hodc->odcl', hidden, out_block, precision=HIGHEST)
    decay = jnp.exp(-relative[None, :] * rate_block[:, None])
    return filter_taps * decay


def reference(tokens, w_value, w_gate_one, w_gate_two, short_taps, filter_in, filter_mid, filter_out, decay_rate, skip, w_out):
    projected = jnp.stack([jnp.dot(tokens, weight.T, preferred_element_type=jnp.float32).astype(jnp.bfloat16)
                           for weight in (w_value, w_gate_one, w_gate_two)])
    projected = lax.optimization_barrier(projected).astype(jnp.float32)
    padded = jnp.pad(projected, ((0, 0), (1, 1), (0, 0)))
    shorted = (padded[:, :-2] * short_taps[:, 0][:, None, :] + padded[:, 1:-1] * short_taps[:, 1][:, None, :]
               + padded[:, 2:] * short_taps[:, 2][:, None, :])
    n_blocks = HW // 128
    inputs = shorted.reshape(3, SEQ, n_blocks, 128).transpose(2, 0, 3, 1)
    out_blocks = filter_out.reshape(FILTER_HID, 2, 2, n_blocks, 128).transpose(3, 0, 1, 2, 4)
    rate_blocks = decay_rate.reshape(n_blocks, 128)
    skip_blocks = skip.reshape(2, n_blocks, 128).transpose(1, 0, 2)

    def mix_block(packed):
        block_in, out_block, rate_block, skip_block = packed
        filter_taps = filter_bank(filter_in, filter_mid, out_block, rate_block)
        forward_part = filter_taps[:, 0]
        backward_part = filter_taps[:, 1]
        kern = jnp.concatenate([forward_part, jnp.zeros(forward_part[..., :1].shape, jnp.float32),
                                backward_part[..., 1:][..., ::-1]], axis=-1)
        spectrum = jnp.fft.rfft(kern, axis=-1)
        signal = block_in[0]
        for order_index in range(2):
            signal_freq = jnp.fft.rfft(signal, n=2 * SEQ, axis=-1)
            long_part = jnp.fft.irfft(signal_freq * spectrum[order_index], n=2 * SEQ, axis=-1)[..., :SEQ]
            signal = block_in[order_index + 1] * (long_part + skip_block[order_index][:, None] * signal)
        return signal.astype(jnp.bfloat16)

    outputs = lax.map(mix_block, (inputs, out_blocks, rate_blocks, skip_blocks))
    mixer_out = outputs.transpose(2, 0, 1).reshape(SEQ, HW)
    return jnp.dot(mixer_out, w_out, preferred_element_type=jnp.float32).astype(jnp.bfloat16)
```

```python
import functools
import math

import jax
import jax.numpy as jnp
import numpy as np
from jax import lax
from jax.experimental import pallas as pl
from jax.experimental.pallas import tpu as pltpu
from jax.sharding import PartitionSpec as P

BANDS = 16


HIGHEST = lax.Precision.HIGHEST


def tables(row_count, col_count, modulus):
    product = (
        jnp.arange(row_count, dtype=jnp.int32)[:, None]
        * jnp.arange(col_count, dtype=jnp.int32)[None, :]
        % modulus
    )
    angles = product.astype(jnp.float32) * (2 * math.pi / modulus)
    return (jnp.cos(angles), jnp.sin(angles))


def forward_transform(signal, in_count, wide, block_len):
    leading = signal.shape[:-1]
    inner_b = min(block_len, 128)
    inner_a = block_len // inner_b
    shaped = signal.reshape(leading + (in_count, block_len))
    cos_one, sin_one = tables(wide, in_count, wide)
    real_part = jnp.einsum("kn,...nt->...kt", cos_one, shaped, precision=HIGHEST)
    imag_part = -jnp.einsum("kn,...nt->...kt", sin_one, shaped, precision=HIGHEST)
    cos_two, sin_two = tables(wide, block_len, wide * block_len)
    real_part, imag_part = (
        real_part * cos_two + imag_part * sin_two,
        imag_part * cos_two - real_part * sin_two,
    )
    real_part = real_part.reshape(leading + (wide, inner_a, inner_b))
    imag_part = imag_part.reshape(leading + (wide, inner_a, inner_b))
    cos_three, sin_three = tables(inner_a, inner_a, inner_a)
    real_part, imag_part = (
        jnp.einsum("ja,...kab->...kjb", cos_three, real_part, precision=HIGHEST)
        + jnp.einsum("ja,...kab->...kjb", sin_three, imag_part, precision=HIGHEST),
        jnp.einsum("ja,...kab->...kjb", cos_three, imag_part, precision=HIGHEST)
        - jnp.einsum("ja,...kab->...kjb", sin_three, real_part, precision=HIGHEST),
    )
    cos_four, sin_four = tables(inner_a, inner_b, block_len)
    real_part, imag_part = (
        real_part * cos_four + imag_part * sin_four,
        imag_part * cos_four - real_part * sin_four,
    )
    cos_five, sin_five = tables(inner_b, inner_b, inner_b)
    return (
        jnp.einsum("...jb,bm->...jm", real_part, cos_five, precision=HIGHEST)
        + jnp.einsum("...jb,bm->...jm", imag_part, sin_five, precision=HIGHEST),
        jnp.einsum("...jb,bm->...jm", imag_part, cos_five, precision=HIGHEST)
        - jnp.einsum("...jb,bm->...jm", real_part, sin_five, precision=HIGHEST),
    )


def inverse_transform(real_part, imag_part, out_count, wide, block_len):
    leading = real_part.shape[:-3]
    inner_b = min(block_len, 128)
    inner_a = block_len // inner_b
    cos_five, sin_five = tables(inner_b, inner_b, inner_b)
    real_part, imag_part = (
        jnp.einsum("...jm,mb->...jb", real_part, cos_five, precision=HIGHEST)
        - jnp.einsum("...jm,mb->...jb", imag_part, sin_five, precision=HIGHEST),
        jnp.einsum("...jm,mb->...jb", imag_part, cos_five, precision=HIGHEST)
        + jnp.einsum("...jm,mb->...jb", real_part, sin_five, precision=HIGHEST),
    )
    cos_four, sin_four = tables(inner_a, inner_b, block_len)
    real_part, imag_part = (
        real_part * cos_four - imag_part * sin_four,
        imag_part * cos_four + real_part * sin_four,
    )
    cos_three, sin_three = tables(inner_a, inner_a, inner_a)
    real_part, imag_part = (
        jnp.einsum("aj,...kjb->...kab", cos_three, real_part, precision=HIGHEST)
        - jnp.einsum("aj,...kjb->...kab", sin_three, imag_part, precision=HIGHEST),
        jnp.einsum("aj,...kjb->...kab", cos_three, imag_part, precision=HIGHEST)
        + jnp.einsum("aj,...kjb->...kab", sin_three, real_part, precision=HIGHEST),
    )
    real_part = real_part.reshape(leading + (wide, block_len))
    imag_part = imag_part.reshape(leading + (wide, block_len))
    cos_two, sin_two = tables(wide, block_len, wide * block_len)
    real_part, imag_part = (
        real_part * cos_two - imag_part * sin_two,
        imag_part * cos_two + real_part * sin_two,
    )
    cos_one, sin_one = tables(out_count, wide, wide)
    result = jnp.einsum("nk,...kt->...nt", cos_one, real_part, precision=HIGHEST) - jnp.einsum(
        "nk,...kt->...nt", sin_one, imag_part, precision=HIGHEST
    )
    return (result / (wide * block_len)).reshape(leading + (out_count * block_len,))


def short_filter(padded, filter_taps):
    return (
        padded[..., :-2] * filter_taps[:, 0, :, None]
        + padded[..., 1:-1] * filter_taps[:, 1, :, None]
        + padded[..., 2:] * filter_taps[:, 2, :, None]
    )


def filter_bank(seq_len, filter_in, filter_mid, out_block, rate_block):
    positions = jnp.arange(seq_len, dtype=jnp.float32)
    relative = positions / (seq_len - 1)
    bands = jnp.linspace(0.0001, BANDS - 1, BANDS, dtype=jnp.float32)
    angles = 2 * math.pi / seq_len * positions[:, None] * bands[None, :]
    feats = jnp.concatenate([relative[:, None], jnp.cos(angles), jnp.sin(angles)], axis=1)
    hidden = jnp.sin(jnp.dot(feats, filter_in, precision=HIGHEST))
    hidden = jnp.sin(jnp.dot(hidden, filter_mid, precision=HIGHEST))
    filter_taps = jnp.einsum("lh,hodc->odcl", hidden, out_block, precision=HIGHEST)
    decay = jnp.exp(-relative[None, :] * rate_block[:, None])
    return filter_taps * decay


def on_device(
    tokens,
    w_value,
    w_gate_one,
    w_gate_two,
    short_taps,
    filter_in,
    filter_mid,
    filter_out,
    decay_rate,
    skip,
    w_out,
):
    n_rows = lax.axis_size("row")
    row_index = lax.axis_index("row")
    col_index = lax.axis_index("col")
    local_width = w_value.shape[0]
    chan_dev = local_width // n_rows
    projected = jnp.stack(
        [
            jnp.einsum("td,cd->ct", tokens, weight, preferred_element_type=jnp.float32)
            for weight in (w_value, w_gate_one, w_gate_two)
        ]
    ).astype(jnp.bfloat16)
    block_len = projected.shape[2]
    seq_len = n_rows * block_len
    wide = 2 * n_rows
    moved = lax.all_to_all(projected, "row", split_axis=1, concat_axis=2, tiled=True)
    own_taps = lax.dynamic_slice_in_dim(short_taps, row_index * chan_dev, chan_dev, 2)
    bordered = jnp.pad(moved.astype(jnp.float32), ((0, 0), (0, 0), (1, 1)))
    channel_major = short_filter(bordered, own_taps)
    global_start = col_index * local_width + row_index * chan_dev
    own_out = lax.dynamic_slice_in_dim(filter_out, global_start, chan_dev, 3)
    own_rate = lax.dynamic_slice_in_dim(decay_rate, row_index * chan_dev, chan_dev, 0)
    own_skip = lax.dynamic_slice_in_dim(skip, row_index * chan_dev, chan_dev, 1)
    filter_taps = filter_bank(seq_len, filter_in, filter_mid, own_out, own_rate)
    forward_part = filter_taps[:, 0]
    backward_part = filter_taps[:, 1]
    kern = jnp.concatenate(
        [
            forward_part,
            jnp.zeros(forward_part[..., :1].shape, jnp.float32),
            backward_part[..., 1:][..., ::-1],
        ],
        axis=-1,
    )
    kern_real, kern_imag = forward_transform(kern, wide, wide, block_len)
    signal = channel_major[0]
    for order_index in range(2):
        sig_real, sig_imag = forward_transform(signal, n_rows, wide, block_len)
        prod_real = sig_real * kern_real[order_index] - sig_imag * kern_imag[order_index]
        prod_imag = sig_real * kern_imag[order_index] + sig_imag * kern_real[order_index]
        long_part = inverse_transform(prod_real, prod_imag, n_rows, wide, block_len)
        signal = channel_major[order_index + 1] * (
            long_part + own_skip[order_index][:, None] * signal
        )
    mixer_channels = signal.astype(jnp.bfloat16)
    position_major = lax.all_to_all(mixer_channels, "row", split_axis=1, concat_axis=0, tiled=True)
    totals = jnp.einsum(
        "ct,cd->td",
        lax.all_gather(position_major, "col", axis=0, tiled=True),
        w_out,
        preferred_element_type=jnp.float32,
    )
    return totals.astype(jnp.bfloat16)


STEP = 32


def position_features(seq_len):
    positions = np.arange(seq_len, dtype=np.float32)
    relative = positions / np.float32(seq_len - 1)
    bands = np.linspace(0.0001, BANDS - 1, BANDS, dtype=np.float32)
    angles = np.float32(2 * math.pi / seq_len) * positions[None, :] * bands[:, None]
    return np.concatenate([relative[None, :], np.cos(angles), np.sin(angles)], axis=0)


def table_seeds(seq_len):
    odd = 2 * np.arange(seq_len)[None, :] + 1
    coarse = (STEP * np.arange(seq_len // STEP)[:, None] * odd) % (4 * seq_len)
    fine = (np.arange(STEP)[:, None] * odd) % (4 * seq_len)
    unit = math.pi / (2 * seq_len)
    return (
        np.stack([np.cos(coarse * unit), np.sin(coarse * unit)]).astype(np.float32),
        np.stack([np.cos(fine * unit), np.sin(fine * unit)]).astype(np.float32),
    )


def split_dot(left, table, table_dim):
    high = left.astype(jnp.bfloat16)
    low = (left - high.astype(jnp.float32)).astype(jnp.bfloat16)
    both = jnp.concatenate([high, low], axis=0)
    product = lax.dot_general(
        both, table, (((1,), (table_dim,)), ((), ())), preferred_element_type=jnp.float32
    )
    return product[: left.shape[0]] + product[left.shape[0] :]


def exact_dot(left, right, left_dim):
    return lax.dot_general(
        left,
        right,
        (((left_dim,), (0,)), ((), ())),
        precision=HIGHEST,
        preferred_element_type=jnp.float32,
    )


def make_tables(coarse_ref, fine_ref, cos_ref, sin_ref):
    def fill(index, carry):
        cos_a = coarse_ref[0, pl.ds(index, 1), :]
        sin_a = coarse_ref[1, pl.ds(index, 1), :]
        cos_b = fine_ref[0]
        sin_b = fine_ref[1]
        rows = pl.ds(pl.multiple_of(index * STEP, STEP), STEP)
        cos_ref[rows, :] = (cos_a * cos_b - sin_a * sin_b).astype(jnp.bfloat16)
        sin_ref[rows, :] = (sin_a * cos_b + cos_a * sin_b).astype(jnp.bfloat16)
        return carry

    lax.fori_loop(0, cos_ref.shape[0] // STEP, fill, 0)


def own_column(vector, chan_dev):
    width = vector.shape[1]
    lanes = lax.broadcasted_iota(jnp.int32, (chan_dev, width), 1)
    wanted = lax.broadcasted_iota(jnp.int32, (chan_dev, width), 0) + lax.axis_index("row") * chan_dev
    return jnp.sum(jnp.where(lanes == wanted, vector, 0.0), axis=1, keepdims=True)


def kernel_spectra(chan_dev, in_ref, mid_ref, out_ref, rate_ref, feats_ref, cos_ref, sin_ref):
    hidden = jnp.sin(exact_dot(in_ref[...], feats_ref[...], 0))
    hidden = jnp.sin(exact_dot(mid_ref[...], hidden, 0))
    decay = jnp.exp(-feats_ref[0:1, :] * own_column(rate_ref[...], chan_dev))
    not_first = lax.broadcasted_iota(jnp.int32, decay.shape, 1) > 0
    sums, differences = [], []
    for order in range(2):
        ahead = exact_dot(out_ref[order, 0], hidden, 1) * decay
        behind = jnp.where(not_first, exact_dot(out_ref[order, 1], hidden, 1) * decay, 0.0)
        sums.append(ahead + behind)
        differences.append(ahead - behind)
    scale = 1.0 / cos_ref.shape[0]
    kern_cos = split_dot(jnp.concatenate(sums, axis=0), cos_ref[...], 0) * scale
    kern_sin = split_dot(jnp.concatenate(differences, axis=0), sin_ref[...], 0) * scale
    return kern_cos, kern_sin


def short_rows(blocks, short_ref, which, chan_dev):
    joined = jnp.concatenate([block.astype(jnp.float32) for block in blocks], axis=1)
    length = joined.shape[1]
    lanes = lax.broadcasted_iota(jnp.int32, joined.shape, 1)
    before = jnp.where(lanes == 0, 0.0, pltpu.roll(joined, 1, 1))
    after = jnp.where(lanes == length - 1, 0.0, pltpu.roll(joined, length - 1, 1))
    tap = [own_column(short_ref[which, j : j + 1, :], chan_dev) for j in range(3)]
    return before * tap[0] + joined * tap[1] + after * tap[2]


def long_convolutions(signals, spectra, skip_ref, cos_ref, sin_ref, chan_dev):
    kern_cos, kern_sin = spectra
    signal = signals[0]
    for order in range(2):
        rows = slice(order * chan_dev, (order + 1) * chan_dev)
        k_cos, k_sin = kern_cos[rows], kern_sin[rows]
        z_cos = split_dot(signal, cos_ref[...], 0)
        z_sin = split_dot(signal, sin_ref[...], 0)
        long_part = split_dot(z_cos * k_cos - z_sin * k_sin, cos_ref[...], 1) + split_dot(
            z_cos * k_sin + z_sin * k_cos, sin_ref[...], 1
        )
        weight = own_column(skip_ref[order : order + 1, :], chan_dev)
        signal = signals[order + 1] * (long_part + weight * signal)
    return signal


def mix_kernel(
    chan_dev,
    moved_ref,
    short_ref,
    in_ref,
    mid_ref,
    out_ref,
    rate_ref,
    skip_ref,
    feats_ref,
    coarse_ref,
    fine_ref,
    y_ref,
    cos_ref,
    sin_ref,
):
    blocks = moved_ref.shape[0]
    block_len = moved_ref.shape[3]
    make_tables(coarse_ref, fine_ref, cos_ref, sin_ref)
    spectra = kernel_spectra(chan_dev, in_ref, mid_ref, out_ref, rate_ref, feats_ref, cos_ref, sin_ref)
    signals = [
        short_rows([moved_ref[s, which] for s in range(blocks)], short_ref, which, chan_dev)
        for which in range(3)
    ]
    signal = long_convolutions(signals, spectra, skip_ref, cos_ref, sin_ref, chan_dev)
    for s in range(blocks):
        y_ref[s] = signal[:, s * block_len : (s + 1) * block_len].astype(jnp.bfloat16)


def on_device_dense(
    tokens,
    w_value,
    w_gate_one,
    w_gate_two,
    short_taps,
    filter_in,
    filter_mid,
    filter_out,
    decay_rate,
    skip,
    w_out,
):
    n_rows = lax.axis_size("row")
    row_index = lax.axis_index("row")
    col_index = lax.axis_index("col")
    local_width = w_value.shape[0]
    chan_dev = local_width // n_rows
    block_len = tokens.shape[0]
    seq_len = n_rows * block_len
    projected = [
        jnp.einsum("td,cd->ct", tokens, weight, preferred_element_type=jnp.float32)
        .astype(jnp.bfloat16)
        .reshape(n_rows, chan_dev, block_len)
        for weight in (w_value, w_gate_one, w_gate_two)
    ]
    global_start = col_index * local_width + row_index * chan_dev
    own_out = lax.dynamic_slice_in_dim(filter_out, global_start, chan_dev, 3).transpose(1, 2, 3, 0)
    coarse, fine = table_seeds(seq_len)
    moved = lax.all_to_all(jnp.stack(projected, axis=1), "row", split_axis=0, concat_axis=0, tiled=True)
    mixer_channels = pl.pallas_call(
        functools.partial(mix_kernel, chan_dev),
        out_shape=jax.ShapeDtypeStruct((n_rows, chan_dev, block_len), jnp.bfloat16),
        in_specs=[pl.BlockSpec(memory_space=pltpu.VMEM)] * 10,
        out_specs=pl.BlockSpec(memory_space=pltpu.VMEM),
        scratch_shapes=[pltpu.VMEM((seq_len, seq_len), jnp.bfloat16)] * 2,
        compiler_params=pltpu.CompilerParams(vmem_limit_bytes=40 << 20),
    )(
        moved,
        short_taps,
        filter_in,
        filter_mid,
        own_out,
        decay_rate.reshape(1, local_width),
        skip,
        position_features(seq_len),
        coarse,
        fine,
    )
    position_major = lax.all_to_all(mixer_channels, "row", split_axis=0, concat_axis=0, tiled=True)
    totals = jnp.einsum(
        "ct,cd->td",
        lax.all_gather(position_major.reshape(local_width, block_len), "col", axis=0, tiled=True),
        w_out,
        preferred_element_type=jnp.float32,
    )
    return totals.astype(jnp.bfloat16)


def solution(mesh):
    placed = (
        P("row", None),
        P("col", None),
        P("col", None),
        P("col", None),
        P(None, None, "col"),
        P(),
        P(),
        P(),
        P("col"),
        P(None, "col"),
        P(None, "col"),
    )

    def program(tokens, w_value, *rest):
        seq_len = tokens.shape[0]
        devices = mesh.shape["row"] * mesh.shape["col"]
        dense = (
            seq_len <= 2048
            and seq_len // mesh.shape["row"] % 128 == 0
            and w_value.shape[0] // devices % 8 == 0
        )
        body = on_device_dense if dense else on_device
        return jax.shard_map(
            body, mesh=mesh, in_specs=placed, out_specs=P("row", "col"), check_vma=False
        )(tokens, w_value, *rest)

    return program
```

```python
import functools
import math

import jax
import jax.numpy as jnp
import numpy as np
from jax import lax
from jax.experimental import pallas as pl
from jax.experimental.pallas import tpu as pltpu
from jax.sharding import PartitionSpec as P

BANDS = 16


HIGHEST = lax.Precision.HIGHEST


def tables(row_count, col_count, modulus):
    product = (
        jnp.arange(row_count, dtype=jnp.int32)[:, None]
        * jnp.arange(col_count, dtype=jnp.int32)[None, :]
        % modulus
    )
    angles = product.astype(jnp.float32) * (2 * math.pi / modulus)
    return (jnp.cos(angles), jnp.sin(angles))


def forward_transform(signal, in_count, wide, block_len):
    leading = signal.shape[:-1]
    inner_b = min(block_len, 128)
    inner_a = block_len // inner_b
    shaped = signal.reshape(leading + (in_count, block_len))
    cos_one, sin_one = tables(wide, in_count, wide)
    real_part = jnp.einsum("kn,...nt->...kt", cos_one, shaped, precision=HIGHEST)
    imag_part = -jnp.einsum("kn,...nt->...kt", sin_one, shaped, precision=HIGHEST)
    cos_two, sin_two = tables(wide, block_len, wide * block_len)
    real_part, imag_part = (
        real_part * cos_two + imag_part * sin_two,
        imag_part * cos_two - real_part * sin_two,
    )
    real_part = real_part.reshape(leading + (wide, inner_a, inner_b))
    imag_part = imag_part.reshape(leading + (wide, inner_a, inner_b))
    cos_three, sin_three = tables(inner_a, inner_a, inner_a)
    real_part, imag_part = (
        jnp.einsum("ja,...kab->...kjb", cos_three, real_part, precision=HIGHEST)
        + jnp.einsum("ja,...kab->...kjb", sin_three, imag_part, precision=HIGHEST),
        jnp.einsum("ja,...kab->...kjb", cos_three, imag_part, precision=HIGHEST)
        - jnp.einsum("ja,...kab->...kjb", sin_three, real_part, precision=HIGHEST),
    )
    cos_four, sin_four = tables(inner_a, inner_b, block_len)
    real_part, imag_part = (
        real_part * cos_four + imag_part * sin_four,
        imag_part * cos_four - real_part * sin_four,
    )
    cos_five, sin_five = tables(inner_b, inner_b, inner_b)
    return (
        jnp.einsum("...jb,bm->...jm", real_part, cos_five, precision=HIGHEST)
        + jnp.einsum("...jb,bm->...jm", imag_part, sin_five, precision=HIGHEST),
        jnp.einsum("...jb,bm->...jm", imag_part, cos_five, precision=HIGHEST)
        - jnp.einsum("...jb,bm->...jm", real_part, sin_five, precision=HIGHEST),
    )


def inverse_transform(real_part, imag_part, out_count, wide, block_len):
    leading = real_part.shape[:-3]
    inner_b = min(block_len, 128)
    inner_a = block_len // inner_b
    cos_five, sin_five = tables(inner_b, inner_b, inner_b)
    real_part, imag_part = (
        jnp.einsum("...jm,mb->...jb", real_part, cos_five, precision=HIGHEST)
        - jnp.einsum("...jm,mb->...jb", imag_part, sin_five, precision=HIGHEST),
        jnp.einsum("...jm,mb->...jb", imag_part, cos_five, precision=HIGHEST)
        + jnp.einsum("...jm,mb->...jb", real_part, sin_five, precision=HIGHEST),
    )
    cos_four, sin_four = tables(inner_a, inner_b, block_len)
    real_part, imag_part = (
        real_part * cos_four - imag_part * sin_four,
        imag_part * cos_four + real_part * sin_four,
    )
    cos_three, sin_three = tables(inner_a, inner_a, inner_a)
    real_part, imag_part = (
        jnp.einsum("aj,...kjb->...kab", cos_three, real_part, precision=HIGHEST)
        - jnp.einsum("aj,...kjb->...kab", sin_three, imag_part, precision=HIGHEST),
        jnp.einsum("aj,...kjb->...kab", cos_three, imag_part, precision=HIGHEST)
        + jnp.einsum("aj,...kjb->...kab", sin_three, real_part, precision=HIGHEST),
    )
    real_part = real_part.reshape(leading + (wide, block_len))
    imag_part = imag_part.reshape(leading + (wide, block_len))
    cos_two, sin_two = tables(wide, block_len, wide * block_len)
    real_part, imag_part = (
        real_part * cos_two - imag_part * sin_two,
        imag_part * cos_two + real_part * sin_two,
    )
    cos_one, sin_one = tables(out_count, wide, wide)
    result = jnp.einsum("nk,...kt->...nt", cos_one, real_part, precision=HIGHEST) - jnp.einsum(
        "nk,...kt->...nt", sin_one, imag_part, precision=HIGHEST
    )
    return (result / (wide * block_len)).reshape(leading + (out_count * block_len,))


def short_filter(padded, filter_taps):
    return (
        padded[..., :-2] * filter_taps[:, 0, :, None]
        + padded[..., 1:-1] * filter_taps[:, 1, :, None]
        + padded[..., 2:] * filter_taps[:, 2, :, None]
    )


def filter_bank(seq_len, filter_in, filter_mid, out_block, rate_block):
    positions = jnp.arange(seq_len, dtype=jnp.float32)
    relative = positions / (seq_len - 1)
    bands = jnp.linspace(0.0001, BANDS - 1, BANDS, dtype=jnp.float32)
    angles = 2 * math.pi / seq_len * positions[:, None] * bands[None, :]
    feats = jnp.concatenate([relative[:, None], jnp.cos(angles), jnp.sin(angles)], axis=1)
    hidden = jnp.sin(jnp.dot(feats, filter_in, precision=HIGHEST))
    hidden = jnp.sin(jnp.dot(hidden, filter_mid, precision=HIGHEST))
    filter_taps = jnp.einsum("lh,hodc->odcl", hidden, out_block, precision=HIGHEST)
    decay = jnp.exp(-relative[None, :] * rate_block[:, None])
    return filter_taps * decay


def on_device(
    tokens,
    w_value,
    w_gate_one,
    w_gate_two,
    short_taps,
    filter_in,
    filter_mid,
    filter_out,
    decay_rate,
    skip,
    w_out,
):
    n_rows = lax.axis_size("row")
    row_index = lax.axis_index("row")
    col_index = lax.axis_index("col")
    local_width = w_value.shape[0]
    chan_dev = local_width // n_rows
    projected = jnp.stack(
        [
            jnp.einsum("td,cd->ct", tokens, weight, preferred_element_type=jnp.float32)
            for weight in (w_value, w_gate_one, w_gate_two)
        ]
    ).astype(jnp.bfloat16)
    block_len = projected.shape[2]
    seq_len = n_rows * block_len
    wide = 2 * n_rows
    moved = lax.all_to_all(projected, "row", split_axis=1, concat_axis=2, tiled=True)
    own_taps = lax.dynamic_slice_in_dim(short_taps, row_index * chan_dev, chan_dev, 2)
    bordered = jnp.pad(moved.astype(jnp.float32), ((0, 0), (0, 0), (1, 1)))
    channel_major = short_filter(bordered, own_taps)
    global_start = col_index * local_width + row_index * chan_dev
    own_out = lax.dynamic_slice_in_dim(filter_out, global_start, chan_dev, 3)
    own_rate = lax.dynamic_slice_in_dim(decay_rate, row_index * chan_dev, chan_dev, 0)
    own_skip = lax.dynamic_slice_in_dim(skip, row_index * chan_dev, chan_dev, 1)
    filter_taps = filter_bank(seq_len, filter_in, filter_mid, own_out, own_rate)
    forward_part = filter_taps[:, 0]
    backward_part = filter_taps[:, 1]
    kern = jnp.concatenate(
        [
            forward_part,
            jnp.zeros(forward_part[..., :1].shape, jnp.float32),
            backward_part[..., 1:][..., ::-1],
        ],
        axis=-1,
    )
    kern_real, kern_imag = forward_transform(kern, wide, wide, block_len)
    signal = channel_major[0]
    for order_index in range(2):
        sig_real, sig_imag = forward_transform(signal, n_rows, wide, block_len)
        prod_real = sig_real * kern_real[order_index] - sig_imag * kern_imag[order_index]
        prod_imag = sig_real * kern_imag[order_index] + sig_imag * kern_real[order_index]
        long_part = inverse_transform(prod_real, prod_imag, n_rows, wide, block_len)
        signal = channel_major[order_index + 1] * (
            long_part + own_skip[order_index][:, None] * signal
        )
    mixer_channels = signal.astype(jnp.bfloat16)
    position_major = lax.all_to_all(mixer_channels, "row", split_axis=1, concat_axis=0, tiled=True)
    totals = jnp.einsum(
        "ct,cd->td",
        lax.all_gather(position_major, "col", axis=0, tiled=True),
        w_out,
        preferred_element_type=jnp.float32,
    )
    return totals.astype(jnp.bfloat16)


STEP = 32


def position_features(seq_len):
    positions = np.arange(seq_len, dtype=np.float32)
    relative = positions / np.float32(seq_len - 1)
    bands = np.linspace(0.0001, BANDS - 1, BANDS, dtype=np.float32)
    angles = np.float32(2 * math.pi / seq_len) * positions[None, :] * bands[:, None]
    return np.concatenate([relative[None, :], np.cos(angles), np.sin(angles)], axis=0)


def table_seeds(seq_len):
    odd = 2 * np.arange(seq_len)[None, :] + 1
    coarse = (STEP * np.arange(seq_len // STEP)[:, None] * odd) % (4 * seq_len)
    fine = (np.arange(STEP)[:, None] * odd) % (4 * seq_len)
    unit = math.pi / (2 * seq_len)
    return (
        np.stack([np.cos(coarse * unit), np.sin(coarse * unit)]).astype(np.float32),
        np.stack([np.cos(fine * unit), np.sin(fine * unit)]).astype(np.float32),
    )


def split_dot(left, table, table_dim):
    high = left.astype(jnp.bfloat16)
    low = (left - high.astype(jnp.float32)).astype(jnp.bfloat16)
    both = jnp.concatenate([high, low], axis=0)
    product = lax.dot_general(
        both, table, (((1,), (table_dim,)), ((), ())), preferred_element_type=jnp.float32
    )
    return product[: left.shape[0]] + product[left.shape[0] :]


def exact_dot(left, right, left_dim):
    return lax.dot_general(
        left,
        right,
        (((left_dim,), (0,)), ((), ())),
        precision=HIGHEST,
        preferred_element_type=jnp.float32,
    )


def make_tables(coarse_ref, fine_ref, cos_ref, sin_ref):
    def fill(index, carry):
        cos_a = coarse_ref[0, pl.ds(index, 1), :]
        sin_a = coarse_ref[1, pl.ds(index, 1), :]
        cos_b = fine_ref[0]
        sin_b = fine_ref[1]
        rows = pl.ds(pl.multiple_of(index * STEP, STEP), STEP)
        cos_ref[rows, :] = (cos_a * cos_b - sin_a * sin_b).astype(jnp.bfloat16)
        sin_ref[rows, :] = (sin_a * cos_b + cos_a * sin_b).astype(jnp.bfloat16)
        return carry

    lax.fori_loop(0, cos_ref.shape[0] // STEP, fill, 0)


def own_column(vector, chan_dev):
    width = vector.shape[1]
    lanes = lax.broadcasted_iota(jnp.int32, (chan_dev, width), 1)
    wanted = lax.broadcasted_iota(jnp.int32, (chan_dev, width), 0) + lax.axis_index("row") * chan_dev
    return jnp.sum(jnp.where(lanes == wanted, vector, 0.0), axis=1, keepdims=True)


def kernel_spectra(chan_dev, in_ref, mid_ref, out_ref, rate_ref, feats_ref, cos_ref, sin_ref):
    hidden = jnp.sin(exact_dot(in_ref[...], feats_ref[...], 0))
    hidden = jnp.sin(exact_dot(mid_ref[...], hidden, 0))
    decay = jnp.exp(-feats_ref[0:1, :] * own_column(rate_ref[...], chan_dev))
    not_first = lax.broadcasted_iota(jnp.int32, decay.shape, 1) > 0
    sums, differences = [], []
    for order in range(2):
        ahead = exact_dot(out_ref[order, 0], hidden, 1) * decay
        behind = jnp.where(not_first, exact_dot(out_ref[order, 1], hidden, 1) * decay, 0.0)
        sums.append(ahead + behind)
        differences.append(ahead - behind)
    scale = 1.0 / cos_ref.shape[0]
    kern_cos = split_dot(jnp.concatenate(sums, axis=0), cos_ref[...], 0) * scale
    kern_sin = split_dot(jnp.concatenate(differences, axis=0), sin_ref[...], 0) * scale
    return kern_cos, kern_sin


def short_rows(blocks, short_ref, which, chan_dev):
    joined = jnp.concatenate([block.astype(jnp.float32) for block in blocks], axis=1)
    length = joined.shape[1]
    lanes = lax.broadcasted_iota(jnp.int32, joined.shape, 1)
    before = jnp.where(lanes == 0, 0.0, pltpu.roll(joined, 1, 1))
    after = jnp.where(lanes == length - 1, 0.0, pltpu.roll(joined, length - 1, 1))
    tap = [own_column(short_ref[which, j : j + 1, :], chan_dev) for j in range(3)]
    return before * tap[0] + joined * tap[1] + after * tap[2]


def long_convolutions(signal_of, spectra, skip_ref, cos_ref, sin_ref, chan_dev):
    kern_cos, kern_sin = spectra
    signal = signal_of(0)
    for order in range(2):
        rows = slice(order * chan_dev, (order + 1) * chan_dev)
        k_cos, k_sin = kern_cos[rows], kern_sin[rows]
        z_cos = split_dot(signal, cos_ref[...], 0)
        z_sin = split_dot(signal, sin_ref[...], 0)
        long_part = split_dot(z_cos * k_cos - z_sin * k_sin, cos_ref[...], 1) + split_dot(
            z_cos * k_sin + z_sin * k_cos, sin_ref[...], 1
        )
        weight = own_column(skip_ref[order : order + 1, :], chan_dev)
        signal = signal_of(order + 1) * (long_part + weight * signal)
    return signal


def mix_kernel(
    n_rows,
    n_cols,
    chan_dev,
    value_ref,
    first_ref,
    second_ref,
    short_ref,
    in_ref,
    mid_ref,
    out_ref,
    rate_ref,
    skip_ref,
    feats_ref,
    coarse_ref,
    fine_ref,
    gathered_ref,
    cos_ref,
    sin_ref,
    moved_ref,
    y_ref,
    there_send,
    there_recv,
    back_send,
    back_recv,
    far_send,
    far_recv,
    mate_send,
    mate_recv,
):
    row = lax.axis_index("row")
    col = lax.axis_index("col")
    block_len = moved_ref.shape[3]
    half = n_cols // 2
    mate = col + 1 - 2 * (col % 2)
    projected = (value_ref, first_ref, second_ref)

    def copy(source, target, send_sem, recv_sem, to_row, to_col):
        return pltpu.make_async_remote_copy(
            src_ref=source,
            dst_ref=target,
            send_sem=send_sem,
            recv_sem=recv_sem,
            device_id=(to_row, to_col),
            device_id_type=pl.DeviceIdType.MESH,
        )

    def row_at(offset):
        return (row + offset) % n_rows

    def far_at(offset):
        return (col + 2 * offset) % n_cols

    partners = [(row_at(d), col) for d in range(1, n_rows)]
    partners += [(row, far_at(h)) for h in range(1, half)] + [(row, mate)]
    barrier = pltpu.get_barrier_semaphore()
    for partner in partners:
        pl.semaphore_signal(barrier, inc=1, device_id=partner, device_id_type=pl.DeviceIdType.MESH)
    pl.semaphore_wait(barrier, len(partners))

    there = {}
    for which in range(3):
        for d in range(1, n_rows):
            there[which, d] = copy(
                projected[which].at[row_at(d)],
                moved_ref.at[which, row],
                there_send.at[which, d - 1],
                there_recv.at[which, d - 1],
                row_at(d),
                col,
            )
            there[which, d].start()
    for which in range(3):
        moved_ref[which, row] = projected[which][row]

    make_tables(coarse_ref, fine_ref, cos_ref, sin_ref)
    spectra = kernel_spectra(chan_dev, in_ref, mid_ref, out_ref, rate_ref, feats_ref, cos_ref, sin_ref)

    def signal_of(which):
        for d in range(1, n_rows):
            there[which, d].wait_recv()
        return short_rows(
            [moved_ref[which, s] for s in range(n_rows)], short_ref, which, chan_dev
        )

    signal = long_convolutions(signal_of, spectra, skip_ref, cos_ref, sin_ref, chan_dev)
    for s in range(n_rows):
        y_ref[s] = signal[:, s * block_len : (s + 1) * block_len].astype(jnp.bfloat16)
    gathered_ref[col, row] = y_ref[row]

    back = {}
    for d in range(1, n_rows):
        back[d] = copy(
            y_ref.at[row_at(d)],
            gathered_ref.at[col, row],
            back_send.at[d - 1],
            back_recv.at[d - 1],
            row_at(d),
            col,
        )
        back[d].start()
    far, near = {}, {}

    def to_mate(h, d):
        block = gathered_ref.at[far_at(h), row_at(n_rows - d)]
        near[h, d] = copy(block, block, mate_send.at[h, d], mate_recv.at[h, d], row, mate)
        near[h, d].start()

    for d in range(n_rows):
        if d:
            back[d].wait_recv()
        block = gathered_ref.at[col, row_at(n_rows - d)]
        for h in range(1, half):
            far[h, d] = copy(
                block, block, far_send.at[h - 1, d], far_recv.at[h - 1, d], row, far_at(h)
            )
            far[h, d].start()
        to_mate(0, d)
    for h in range(1, half):
        for d in range(n_rows):
            far[h, d].wait_recv()
            to_mate(half - h, d)
    for send in (there, back, far, near):
        for one in send.values():
            one.wait_send()
    for one in near.values():
        one.wait_recv()


def on_device_dense(
    tokens,
    w_value,
    w_gate_one,
    w_gate_two,
    short_taps,
    filter_in,
    filter_mid,
    filter_out,
    decay_rate,
    skip,
    w_out,
):
    n_rows = lax.axis_size("row")
    row_index = lax.axis_index("row")
    col_index = lax.axis_index("col")
    local_width = w_value.shape[0]
    chan_dev = local_width // n_rows
    block_len = tokens.shape[0]
    seq_len = n_rows * block_len
    projected = [
        jnp.einsum("td,cd->ct", tokens, weight, preferred_element_type=jnp.float32)
        .astype(jnp.bfloat16)
        .reshape(n_rows, chan_dev, block_len)
        for weight in (w_value, w_gate_one, w_gate_two)
    ]
    global_start = col_index * local_width + row_index * chan_dev
    own_out = lax.dynamic_slice_in_dim(filter_out, global_start, chan_dev, 3).transpose(1, 2, 3, 0)
    coarse, fine = table_seeds(seq_len)
    n_cols = lax.axis_size("col")
    half = n_cols // 2
    dma = pltpu.SemaphoreType.DMA
    gathered = pl.pallas_call(
        functools.partial(mix_kernel, n_rows, n_cols, chan_dev),
        out_shape=jax.ShapeDtypeStruct((n_cols, n_rows, chan_dev, block_len), jnp.bfloat16),
        in_specs=[pl.BlockSpec(memory_space=pltpu.VMEM)] * 12,
        out_specs=pl.BlockSpec(memory_space=pltpu.VMEM),
        scratch_shapes=[
            pltpu.VMEM((seq_len, seq_len), jnp.bfloat16),
            pltpu.VMEM((seq_len, seq_len), jnp.bfloat16),
            pltpu.VMEM((3, n_rows, chan_dev, block_len), jnp.bfloat16),
            pltpu.VMEM((n_rows, chan_dev, block_len), jnp.bfloat16),
            dma((3, n_rows - 1)),
            dma((3, n_rows - 1)),
            dma((n_rows - 1,)),
            dma((n_rows - 1,)),
            dma((half - 1, n_rows)),
            dma((half - 1, n_rows)),
            dma((half, n_rows)),
            dma((half, n_rows)),
        ],
        compiler_params=pltpu.CompilerParams(
            vmem_limit_bytes=26 << 20, collective_id=0, has_side_effects=True
        ),
    )(
        *projected,
        short_taps,
        filter_in,
        filter_mid,
        own_out,
        decay_rate.reshape(1, local_width),
        skip,
        position_features(seq_len),
        coarse,
        fine,
    )
    totals = jnp.einsum(
        "ct,cd->td",
        gathered.reshape(n_cols * local_width, block_len),
        w_out,
        preferred_element_type=jnp.float32,
    )
    return totals.astype(jnp.bfloat16)


def solution(mesh):
    placed = (
        P("row", None),
        P("col", None),
        P("col", None),
        P("col", None),
        P(None, None, "col"),
        P(),
        P(),
        P(),
        P("col"),
        P(None, "col"),
        P(None, "col"),
    )

    def program(tokens, w_value, *rest):
        seq_len = tokens.shape[0]
        devices = mesh.shape["row"] * mesh.shape["col"]
        columns = mesh.shape["col"]
        dense = (
            seq_len <= 2048
            and seq_len // mesh.shape["row"] % 128 == 0
            and w_value.shape[0] // devices % 8 == 0
            and columns % 2 == 0
            and columns > 2
        )
        body = on_device_dense if dense else on_device
        return jax.shard_map(
            body, mesh=mesh, in_specs=placed, out_specs=P("row", "col"), check_vma=False
        )(tokens, w_value, *rest)

    return program
```

```python
import functools
import math

import jax
import jax.numpy as jnp
import numpy as np
from jax import lax
from jax.experimental import pallas as pl
from jax.experimental.pallas import tpu as pltpu
from jax.sharding import PartitionSpec as P

BANDS = 16


HIGHEST = lax.Precision.HIGHEST


def tables(row_count, col_count, modulus):
    product = (
        jnp.arange(row_count, dtype=jnp.int32)[:, None]
        * jnp.arange(col_count, dtype=jnp.int32)[None, :]
        % modulus
    )
    angles = product.astype(jnp.float32) * (2 * math.pi / modulus)
    return (jnp.cos(angles), jnp.sin(angles))


def forward_transform(signal, in_count, wide, block_len):
    leading = signal.shape[:-1]
    inner_b = min(block_len, 128)
    inner_a = block_len // inner_b
    shaped = signal.reshape(leading + (in_count, block_len))
    cos_one, sin_one = tables(wide, in_count, wide)
    real_part = jnp.einsum("kn,...nt->...kt", cos_one, shaped, precision=HIGHEST)
    imag_part = -jnp.einsum("kn,...nt->...kt", sin_one, shaped, precision=HIGHEST)
    cos_two, sin_two = tables(wide, block_len, wide * block_len)
    real_part, imag_part = (
        real_part * cos_two + imag_part * sin_two,
        imag_part * cos_two - real_part * sin_two,
    )
    real_part = real_part.reshape(leading + (wide, inner_a, inner_b))
    imag_part = imag_part.reshape(leading + (wide, inner_a, inner_b))
    cos_three, sin_three = tables(inner_a, inner_a, inner_a)
    real_part, imag_part = (
        jnp.einsum("ja,...kab->...kjb", cos_three, real_part, precision=HIGHEST)
        + jnp.einsum("ja,...kab->...kjb", sin_three, imag_part, precision=HIGHEST),
        jnp.einsum("ja,...kab->...kjb", cos_three, imag_part, precision=HIGHEST)
        - jnp.einsum("ja,...kab->...kjb", sin_three, real_part, precision=HIGHEST),
    )
    cos_four, sin_four = tables(inner_a, inner_b, block_len)
    real_part, imag_part = (
        real_part * cos_four + imag_part * sin_four,
        imag_part * cos_four - real_part * sin_four,
    )
    cos_five, sin_five = tables(inner_b, inner_b, inner_b)
    return (
        jnp.einsum("...jb,bm->...jm", real_part, cos_five, precision=HIGHEST)
        + jnp.einsum("...jb,bm->...jm", imag_part, sin_five, precision=HIGHEST),
        jnp.einsum("...jb,bm->...jm", imag_part, cos_five, precision=HIGHEST)
        - jnp.einsum("...jb,bm->...jm", real_part, sin_five, precision=HIGHEST),
    )


def inverse_transform(real_part, imag_part, out_count, wide, block_len):
    leading = real_part.shape[:-3]
    inner_b = min(block_len, 128)
    inner_a = block_len // inner_b
    cos_five, sin_five = tables(inner_b, inner_b, inner_b)
    real_part, imag_part = (
        jnp.einsum("...jm,mb->...jb", real_part, cos_five, precision=HIGHEST)
        - jnp.einsum("...jm,mb->...jb", imag_part, sin_five, precision=HIGHEST),
        jnp.einsum("...jm,mb->...jb", imag_part, cos_five, precision=HIGHEST)
        + jnp.einsum("...jm,mb->...jb", real_part, sin_five, precision=HIGHEST),
    )
    cos_four, sin_four = tables(inner_a, inner_b, block_len)
    real_part, imag_part = (
        real_part * cos_four - imag_part * sin_four,
        imag_part * cos_four + real_part * sin_four,
    )
    cos_three, sin_three = tables(inner_a, inner_a, inner_a)
    real_part, imag_part = (
        jnp.einsum("aj,...kjb->...kab", cos_three, real_part, precision=HIGHEST)
        - jnp.einsum("aj,...kjb->...kab", sin_three, imag_part, precision=HIGHEST),
        jnp.einsum("aj,...kjb->...kab", cos_three, imag_part, precision=HIGHEST)
        + jnp.einsum("aj,...kjb->...kab", sin_three, real_part, precision=HIGHEST),
    )
    real_part = real_part.reshape(leading + (wide, block_len))
    imag_part = imag_part.reshape(leading + (wide, block_len))
    cos_two, sin_two = tables(wide, block_len, wide * block_len)
    real_part, imag_part = (
        real_part * cos_two - imag_part * sin_two,
        imag_part * cos_two + real_part * sin_two,
    )
    cos_one, sin_one = tables(out_count, wide, wide)
    result = jnp.einsum("nk,...kt->...nt", cos_one, real_part, precision=HIGHEST) - jnp.einsum(
        "nk,...kt->...nt", sin_one, imag_part, precision=HIGHEST
    )
    return (result / (wide * block_len)).reshape(leading + (out_count * block_len,))


def short_filter(padded, filter_taps):
    return (
        padded[..., :-2] * filter_taps[:, 0, :, None]
        + padded[..., 1:-1] * filter_taps[:, 1, :, None]
        + padded[..., 2:] * filter_taps[:, 2, :, None]
    )


def filter_bank(seq_len, filter_in, filter_mid, out_block, rate_block):
    positions = jnp.arange(seq_len, dtype=jnp.float32)
    relative = positions / (seq_len - 1)
    bands = jnp.linspace(0.0001, BANDS - 1, BANDS, dtype=jnp.float32)
    angles = 2 * math.pi / seq_len * positions[:, None] * bands[None, :]
    feats = jnp.concatenate([relative[:, None], jnp.cos(angles), jnp.sin(angles)], axis=1)
    hidden = jnp.sin(jnp.dot(feats, filter_in, precision=HIGHEST))
    hidden = jnp.sin(jnp.dot(hidden, filter_mid, precision=HIGHEST))
    filter_taps = jnp.einsum("lh,hodc->odcl", hidden, out_block, precision=HIGHEST)
    decay = jnp.exp(-relative[None, :] * rate_block[:, None])
    return filter_taps * decay


def on_device(
    tokens,
    w_value,
    w_gate_one,
    w_gate_two,
    short_taps,
    filter_in,
    filter_mid,
    filter_out,
    decay_rate,
    skip,
    w_out,
):
    n_rows = lax.axis_size("row")
    row_index = lax.axis_index("row")
    col_index = lax.axis_index("col")
    local_width = w_value.shape[0]
    chan_dev = local_width // n_rows
    projected = jnp.stack(
        [
            jnp.einsum("td,cd->ct", tokens, weight, preferred_element_type=jnp.float32)
            for weight in (w_value, w_gate_one, w_gate_two)
        ]
    ).astype(jnp.bfloat16)
    block_len = projected.shape[2]
    seq_len = n_rows * block_len
    wide = 2 * n_rows
    moved = lax.all_to_all(projected, "row", split_axis=1, concat_axis=2, tiled=True)
    own_taps = lax.dynamic_slice_in_dim(short_taps, row_index * chan_dev, chan_dev, 2)
    bordered = jnp.pad(moved.astype(jnp.float32), ((0, 0), (0, 0), (1, 1)))
    channel_major = short_filter(bordered, own_taps)
    global_start = col_index * local_width + row_index * chan_dev
    own_out = lax.dynamic_slice_in_dim(filter_out, global_start, chan_dev, 3)
    own_rate = lax.dynamic_slice_in_dim(decay_rate, row_index * chan_dev, chan_dev, 0)
    own_skip = lax.dynamic_slice_in_dim(skip, row_index * chan_dev, chan_dev, 1)
    filter_taps = filter_bank(seq_len, filter_in, filter_mid, own_out, own_rate)
    forward_part = filter_taps[:, 0]
    backward_part = filter_taps[:, 1]
    kern = jnp.concatenate(
        [
            forward_part,
            jnp.zeros(forward_part[..., :1].shape, jnp.float32),
            backward_part[..., 1:][..., ::-1],
        ],
        axis=-1,
    )
    kern_real, kern_imag = forward_transform(kern, wide, wide, block_len)
    signal = channel_major[0]
    for order_index in range(2):
        sig_real, sig_imag = forward_transform(signal, n_rows, wide, block_len)
        prod_real = sig_real * kern_real[order_index] - sig_imag * kern_imag[order_index]
        prod_imag = sig_real * kern_imag[order_index] + sig_imag * kern_real[order_index]
        long_part = inverse_transform(prod_real, prod_imag, n_rows, wide, block_len)
        signal = channel_major[order_index + 1] * (
            long_part + own_skip[order_index][:, None] * signal
        )
    mixer_channels = signal.astype(jnp.bfloat16)
    position_major = lax.all_to_all(mixer_channels, "row", split_axis=1, concat_axis=0, tiled=True)
    totals = jnp.einsum(
        "ct,cd->td",
        lax.all_gather(position_major, "col", axis=0, tiled=True),
        w_out,
        preferred_element_type=jnp.float32,
    )
    return totals.astype(jnp.bfloat16)


STEP = 32


def position_features(seq_len):
    positions = np.arange(seq_len, dtype=np.float32)
    relative = positions / np.float32(seq_len - 1)
    bands = np.linspace(0.0001, BANDS - 1, BANDS, dtype=np.float32)
    angles = np.float32(2 * math.pi / seq_len) * positions[None, :] * bands[:, None]
    return np.concatenate([relative[None, :], np.cos(angles), np.sin(angles)], axis=0)


def table_seeds(seq_len):
    odd = 2 * np.arange(seq_len)[None, :] + 1
    coarse = (STEP * np.arange(seq_len // STEP)[:, None] * odd) % (4 * seq_len)
    fine = (np.arange(STEP)[:, None] * odd) % (4 * seq_len)
    unit = math.pi / (2 * seq_len)
    return (
        np.stack([np.cos(coarse * unit), np.sin(coarse * unit)]).astype(np.float32),
        np.stack([np.cos(fine * unit), np.sin(fine * unit)]).astype(np.float32),
    )


def split_dot(left, table, table_dim):
    high = left.astype(jnp.bfloat16)
    low = (left - high.astype(jnp.float32)).astype(jnp.bfloat16)
    both = jnp.concatenate([high, low], axis=0)
    product = lax.dot_general(
        both, table, (((1,), (table_dim,)), ((), ())), preferred_element_type=jnp.float32
    )
    return product[: left.shape[0]] + product[left.shape[0] :]


def exact_dot(left, right, left_dim):
    return lax.dot_general(
        left,
        right,
        (((left_dim,), (0,)), ((), ())),
        precision=HIGHEST,
        preferred_element_type=jnp.float32,
    )


def make_tables(coarse_ref, fine_ref, cos_ref, sin_ref):
    def fill(index, carry):
        cos_a = coarse_ref[0, pl.ds(index, 1), :]
        sin_a = coarse_ref[1, pl.ds(index, 1), :]
        cos_b = fine_ref[0]
        sin_b = fine_ref[1]
        rows = pl.ds(pl.multiple_of(index * STEP, STEP), STEP)
        cos_ref[rows, :] = (cos_a * cos_b - sin_a * sin_b).astype(jnp.bfloat16)
        sin_ref[rows, :] = (sin_a * cos_b + cos_a * sin_b).astype(jnp.bfloat16)
        return carry

    lax.fori_loop(0, cos_ref.shape[0] // STEP, fill, 0)


def own_column(vector, chan_dev):
    width = vector.shape[1]
    lanes = lax.broadcasted_iota(jnp.int32, (chan_dev, width), 1)
    wanted = lax.broadcasted_iota(jnp.int32, (chan_dev, width), 0) + lax.axis_index("row") * chan_dev
    return jnp.sum(jnp.where(lanes == wanted, vector, 0.0), axis=1, keepdims=True)


def window_tile(chan_dev, total_width):
    start = (lax.axis_index("col") * lax.axis_size("row") + lax.axis_index("row")) * chan_dev
    tile = start // 128
    return tile - tile // (total_width // 128 - 1), start


def window_picks(chan_dev, total_width, window):
    tile, start = window_tile(chan_dev, total_width)
    lanes = lax.broadcasted_iota(jnp.int32, (chan_dev, window), 1)
    wanted = lax.broadcasted_iota(jnp.int32, (chan_dev, window), 0) + (start - tile * 128)
    return jnp.where(lanes == wanted, 1.0, 0.0)


def kernel_spectra(chan_dev, total_width, in_ref, mid_ref, out_ref, rate_ref, feats_ref, cos_ref, sin_ref):
    hidden = jnp.sin(exact_dot(in_ref[...], feats_ref[...], 0))
    hidden = jnp.sin(exact_dot(mid_ref[...], hidden, 0))
    decay = jnp.exp(-feats_ref[0:1, :] * own_column(rate_ref[...], chan_dev))
    not_first = lax.broadcasted_iota(jnp.int32, decay.shape, 1) > 0
    sums, differences = [], []
    picks = window_picks(chan_dev, total_width, out_ref.shape[3])
    for order in range(2):
        own = [
            lax.dot_general(
                picks,
                out_ref[:, order, direction, :],
                (((1,), (1,)), ((), ())),
                precision=HIGHEST,
                preferred_element_type=jnp.float32,
            )
            for direction in range(2)
        ]
        ahead = exact_dot(own[0], hidden, 1) * decay
        behind = jnp.where(not_first, exact_dot(own[1], hidden, 1) * decay, 0.0)
        sums.append(ahead + behind)
        differences.append(ahead - behind)
    scale = 1.0 / cos_ref.shape[0]
    kern_cos = split_dot(jnp.concatenate(sums, axis=0), cos_ref[...], 0) * scale
    kern_sin = split_dot(jnp.concatenate(differences, axis=0), sin_ref[...], 0) * scale
    return kern_cos, kern_sin


def short_rows(blocks, short_ref, which, chan_dev):
    joined = jnp.concatenate([block.astype(jnp.float32) for block in blocks], axis=1)
    length = joined.shape[1]
    lanes = lax.broadcasted_iota(jnp.int32, joined.shape, 1)
    before = jnp.where(lanes == 0, 0.0, pltpu.roll(joined, 1, 1))
    after = jnp.where(lanes == length - 1, 0.0, pltpu.roll(joined, length - 1, 1))
    tap = [own_column(short_ref[which, j : j + 1, :], chan_dev) for j in range(3)]
    return before * tap[0] + joined * tap[1] + after * tap[2]


def long_convolutions(signal_of, spectra, skip_ref, cos_ref, sin_ref, chan_dev):
    kern_cos, kern_sin = spectra
    signal = signal_of(0)
    for order in range(2):
        rows = slice(order * chan_dev, (order + 1) * chan_dev)
        k_cos, k_sin = kern_cos[rows], kern_sin[rows]
        z_cos = split_dot(signal, cos_ref[...], 0)
        z_sin = split_dot(signal, sin_ref[...], 0)
        long_part = split_dot(z_cos * k_cos - z_sin * k_sin, cos_ref[...], 1) + split_dot(
            z_cos * k_sin + z_sin * k_cos, sin_ref[...], 1
        )
        weight = own_column(skip_ref[order : order + 1, :], chan_dev)
        signal = signal_of(order + 1) * (long_part + weight * signal)
    return signal


def mix_kernel(
    n_rows,
    n_cols,
    chan_dev,
    total_width,
    sources,
    result_ref,
    held,
    cos_ref,
    sin_ref,
    projected_ref,
    moved_ref,
    y_ref,
    gathered,
    load_sem,
    there_send,
    there_recv,
    back_send,
    back_recv,
    far_send,
    far_recv,
    mate_send,
    mate_recv,
):
    row = lax.axis_index("row")
    col = lax.axis_index("col")
    block_len = moved_ref.shape[3]
    half = n_cols // 2
    mate = col + 1 - 2 * (col % 2)
    gathered_ref = result_ref if gathered is None else gathered
    tile, _ = window_tile(chan_dev, total_width)
    lanes = pl.ds(pl.multiple_of(tile * 128, 128), held["filter_out"].shape[3])
    loads = {}
    for index, name in enumerate(sources):
        source = sources[name]
        if name == "filter_out":
            source = source.at[:, :, :, lanes]
        loads[name] = pltpu.make_async_copy(source, held[name], load_sem.at[index])
        loads[name].start()

    def copy(source, target, send_sem, recv_sem, to_row, to_col):
        return pltpu.make_async_remote_copy(
            src_ref=source,
            dst_ref=target,
            send_sem=send_sem,
            recv_sem=recv_sem,
            device_id=(to_row, to_col),
            device_id_type=pl.DeviceIdType.MESH,
        )

    def row_at(offset):
        return (row + offset) % n_rows

    def far_at(offset):
        return (col + 2 * offset) % n_cols

    partners = [(row_at(d), col) for d in range(1, n_rows)]
    partners += [(row, far_at(h)) for h in range(1, half)] + [(row, mate)]
    barrier = pltpu.get_barrier_semaphore()
    for partner in partners:
        pl.semaphore_signal(barrier, inc=1, device_id=partner, device_id_type=pl.DeviceIdType.MESH)
    for name in ("coarse", "fine"):
        loads[name].wait()
    make_tables(held["coarse"], held["fine"], cos_ref, sin_ref)
    loads["tokens"].wait()

    there = {}
    for which, name in enumerate(("w_value", "w_first", "w_second")):
        loads[name].wait()
        rows = held[name].shape[0] // 2
        for part in range(2):
            product = lax.dot_general(
                held[name][part * rows : (part + 1) * rows, :],
                held["tokens"][...],
                (((1,), (1,)), ((), ())),
                preferred_element_type=jnp.float32,
            )
            blocks = n_rows // 2
            for s in range(blocks):
                projected_ref[which, part * blocks + s] = product[
                    s * chan_dev : (s + 1) * chan_dev
                ].astype(jnp.bfloat16)
        moved_ref[which, row] = projected_ref[which, row]
        if which == 0:
            pl.semaphore_wait(barrier, len(partners))
        for d in range(1, n_rows):
            there[which, d] = copy(
                projected_ref.at[which, row_at(d)],
                moved_ref.at[which, row],
                there_send.at[which, d - 1],
                there_recv.at[which, d - 1],
                row_at(d),
                col,
            )
            there[which, d].start()

    for name in ("filter_in", "filter_mid", "filter_out", "rate", "feats", "short_taps", "skip"):
        loads[name].wait()
    spectra = kernel_spectra(
        chan_dev,
        total_width,
        held["filter_in"],
        held["filter_mid"],
        held["filter_out"],
        held["rate"],
        held["feats"],
        cos_ref,
        sin_ref,
    )

    def signal_of(which):
        for d in range(1, n_rows):
            there[which, d].wait_recv()
        return short_rows(
            [moved_ref[which, s] for s in range(n_rows)], held["short_taps"], which, chan_dev
        )

    signal = long_convolutions(signal_of, spectra, held["skip"], cos_ref, sin_ref, chan_dev)
    for s in range(n_rows):
        y_ref[s] = signal[:, s * block_len : (s + 1) * block_len].astype(jnp.bfloat16)
    gathered_ref[col, row] = y_ref[row]

    back = {}
    for d in range(1, n_rows):
        back[d] = copy(
            y_ref.at[row_at(d)],
            gathered_ref.at[col, row],
            back_send.at[d - 1],
            back_recv.at[d - 1],
            row_at(d),
            col,
        )
        back[d].start()
    far, near = {}, {}

    def to_mate(h, d):
        block = gathered_ref.at[far_at(h), row_at(n_rows - d)]
        near[h, d] = copy(block, block, mate_send.at[h, d], mate_recv.at[h, d], row, mate)
        near[h, d].start()

    for d in range(n_rows):
        if d:
            back[d].wait_recv()
        block = gathered_ref.at[col, row_at(n_rows - d)]
        for h in range(1, half):
            far[h, d] = copy(
                block, block, far_send.at[h - 1, d], far_recv.at[h - 1, d], row, far_at(h)
            )
            far[h, d].start()
        to_mate(0, d)
    group = n_rows * chan_dev

    def add_group(owner, total):
        left = jnp.concatenate(
            [gathered_ref[owner, s].astype(jnp.float32) for s in range(n_rows)], axis=0
        ).astype(jnp.bfloat16)
        rows = pl.ds(pl.multiple_of(owner * group, group), group)
        product = lax.dot_general(
            left,
            held["w_out"][rows, :],
            (((0,), (0,)), ((), ())),
            preferred_element_type=jnp.float32,
        )
        return product if total is None else total + product

    loads["w_out"].wait()
    total = add_group(col, None)
    for h in range(1, half):
        for d in range(n_rows):
            far[h, d].wait_recv()
            to_mate(half - h, d)
    for h in range(half):
        if h:
            total = add_group(far_at(h), total)
        for d in range(n_rows):
            near[h, d].wait_recv()
        total = add_group((mate + 2 * h) % n_cols, total)
    result_ref[...] = total.astype(jnp.bfloat16)
    for send in (there, back, far, near):
        for one in send.values():
            one.wait_send()


def on_device_dense(
    tokens,
    w_value,
    w_gate_one,
    w_gate_two,
    short_taps,
    filter_in,
    filter_mid,
    filter_out,
    decay_rate,
    skip,
    w_out,
):
    n_rows = lax.axis_size("row")
    n_cols = lax.axis_size("col")
    half = n_cols // 2
    local_width = w_value.shape[0]
    chan_dev = local_width // n_rows
    total_width = filter_out.shape[3]
    block_len = tokens.shape[0]
    seq_len = n_rows * block_len
    coarse, fine = table_seeds(seq_len)
    sources = dict(
        tokens=tokens,
        coarse=coarse,
        fine=fine,
        w_value=w_value,
        w_first=w_gate_one,
        w_second=w_gate_two,
        filter_out=filter_out,
        filter_in=filter_in,
        filter_mid=filter_mid,
        rate=decay_rate.reshape(1, local_width),
        feats=position_features(seq_len),
        short_taps=short_taps,
        skip=skip,
        w_out=w_out,
    )
    window = -(-(chan_dev + 127) // 128) * 128
    held = {name: pltpu.VMEM(source.shape, source.dtype) for name, source in sources.items()}
    held["filter_out"] = pltpu.VMEM(filter_out.shape[:3] + (window,), filter_out.dtype)
    dma = pltpu.SemaphoreType.DMA
    collected = (n_cols, n_rows, chan_dev, block_len)
    result = jax.ShapeDtypeStruct((block_len, w_out.shape[1]), jnp.bfloat16)
    gathered = pltpu.VMEM(collected, jnp.bfloat16)
    return_value = pl.pallas_call(
        functools.partial(mix_kernel, n_rows, n_cols, chan_dev, total_width),
        out_shape=result,
        in_specs=[{name: pl.BlockSpec(memory_space=pl.ANY) for name in sources}],
        out_specs=pl.BlockSpec(memory_space=pltpu.VMEM),
        scratch_shapes=[
            held,
            pltpu.VMEM((seq_len, seq_len), jnp.bfloat16),
            pltpu.VMEM((seq_len, seq_len), jnp.bfloat16),
            pltpu.VMEM((3, n_rows, chan_dev, block_len), jnp.bfloat16),
            pltpu.VMEM((3, n_rows, chan_dev, block_len), jnp.bfloat16),
            pltpu.VMEM((n_rows, chan_dev, block_len), jnp.bfloat16),
            gathered,
            dma((len(sources),)),
            dma((3, n_rows - 1)),
            dma((3, n_rows - 1)),
            dma((n_rows - 1,)),
            dma((n_rows - 1,)),
            dma((half - 1, n_rows)),
            dma((half - 1, n_rows)),
            dma((half, n_rows)),
            dma((half, n_rows)),
        ],
        compiler_params=pltpu.CompilerParams(
            vmem_limit_bytes=56 << 20, collective_id=0, has_side_effects=True
        ),
    )(sources)
    return return_value


def solution(mesh):
    placed = (
        P("row", None),
        P("col", None),
        P("col", None),
        P("col", None),
        P(None, None, "col"),
        P(),
        P(),
        P(),
        P("col"),
        P(None, "col"),
        P(None, "col"),
    )

    def program(tokens, w_value, *rest):
        seq_len = tokens.shape[0]
        devices = mesh.shape["row"] * mesh.shape["col"]
        columns = mesh.shape["col"]
        dense = (
            seq_len <= 2048
            and seq_len // mesh.shape["row"] % 128 == 0
            and w_value.shape[0] // devices % 8 == 0
            and columns % 2 == 0
            and columns > 2
            and mesh.shape["row"] % 2 == 0
            and rest[5].shape[3] % 128 == 0
            and w_value.shape[0] // devices <= 129
            and rest[5].shape[3] >= 384
        )
        body = on_device_dense if dense else on_device
        return jax.shard_map(
            body, mesh=mesh, in_specs=placed, out_specs=P("row", "col"), check_vma=False
        )(tokens, w_value, *rest)

    return program
```

```python
import functools
import math

import jax
import jax.numpy as jnp
import numpy as np
from jax import lax
from jax.experimental import pallas as pl
from jax.experimental.pallas import tpu as pltpu
from jax.sharding import PartitionSpec as P

BANDS = 16


HIGHEST = lax.Precision.HIGHEST


def tables(row_count, col_count, modulus):
    product = (
        jnp.arange(row_count, dtype=jnp.int32)[:, None]
        * jnp.arange(col_count, dtype=jnp.int32)[None, :]
        % modulus
    )
    angles = product.astype(jnp.float32) * (2 * math.pi / modulus)
    return (jnp.cos(angles), jnp.sin(angles))


def forward_transform(signal, in_count, wide, block_len):
    leading = signal.shape[:-1]
    inner_b = min(block_len, 128)
    inner_a = block_len // inner_b
    shaped = signal.reshape(leading + (in_count, block_len))
    cos_one, sin_one = tables(wide, in_count, wide)
    real_part = jnp.einsum("kn,...nt->...kt", cos_one, shaped, precision=HIGHEST)
    imag_part = -jnp.einsum("kn,...nt->...kt", sin_one, shaped, precision=HIGHEST)
    cos_two, sin_two = tables(wide, block_len, wide * block_len)
    real_part, imag_part = (
        real_part * cos_two + imag_part * sin_two,
        imag_part * cos_two - real_part * sin_two,
    )
    real_part = real_part.reshape(leading + (wide, inner_a, inner_b))
    imag_part = imag_part.reshape(leading + (wide, inner_a, inner_b))
    cos_three, sin_three = tables(inner_a, inner_a, inner_a)
    real_part, imag_part = (
        jnp.einsum("ja,...kab->...kjb", cos_three, real_part, precision=HIGHEST)
        + jnp.einsum("ja,...kab->...kjb", sin_three, imag_part, precision=HIGHEST),
        jnp.einsum("ja,...kab->...kjb", cos_three, imag_part, precision=HIGHEST)
        - jnp.einsum("ja,...kab->...kjb", sin_three, real_part, precision=HIGHEST),
    )
    cos_four, sin_four = tables(inner_a, inner_b, block_len)
    real_part, imag_part = (
        real_part * cos_four + imag_part * sin_four,
        imag_part * cos_four - real_part * sin_four,
    )
    cos_five, sin_five = tables(inner_b, inner_b, inner_b)
    return (
        jnp.einsum("...jb,bm->...jm", real_part, cos_five, precision=HIGHEST)
        + jnp.einsum("...jb,bm->...jm", imag_part, sin_five, precision=HIGHEST),
        jnp.einsum("...jb,bm->...jm", imag_part, cos_five, precision=HIGHEST)
        - jnp.einsum("...jb,bm->...jm", real_part, sin_five, precision=HIGHEST),
    )


def inverse_transform(real_part, imag_part, out_count, wide, block_len):
    leading = real_part.shape[:-3]
    inner_b = min(block_len, 128)
    inner_a = block_len // inner_b
    cos_five, sin_five = tables(inner_b, inner_b, inner_b)
    real_part, imag_part = (
        jnp.einsum("...jm,mb->...jb", real_part, cos_five, precision=HIGHEST)
        - jnp.einsum("...jm,mb->...jb", imag_part, sin_five, precision=HIGHEST),
        jnp.einsum("...jm,mb->...jb", imag_part, cos_five, precision=HIGHEST)
        + jnp.einsum("...jm,mb->...jb", real_part, sin_five, precision=HIGHEST),
    )
    cos_four, sin_four = tables(inner_a, inner_b, block_len)
    real_part, imag_part = (
        real_part * cos_four - imag_part * sin_four,
        imag_part * cos_four + real_part * sin_four,
    )
    cos_three, sin_three = tables(inner_a, inner_a, inner_a)
    real_part, imag_part = (
        jnp.einsum("aj,...kjb->...kab", cos_three, real_part, precision=HIGHEST)
        - jnp.einsum("aj,...kjb->...kab", sin_three, imag_part, precision=HIGHEST),
        jnp.einsum("aj,...kjb->...kab", cos_three, imag_part, precision=HIGHEST)
        + jnp.einsum("aj,...kjb->...kab", sin_three, real_part, precision=HIGHEST),
    )
    real_part = real_part.reshape(leading + (wide, block_len))
    imag_part = imag_part.reshape(leading + (wide, block_len))
    cos_two, sin_two = tables(wide, block_len, wide * block_len)
    real_part, imag_part = (
        real_part * cos_two - imag_part * sin_two,
        imag_part * cos_two + real_part * sin_two,
    )
    cos_one, sin_one = tables(out_count, wide, wide)
    result = jnp.einsum("nk,...kt->...nt", cos_one, real_part, precision=HIGHEST) - jnp.einsum(
        "nk,...kt->...nt", sin_one, imag_part, precision=HIGHEST
    )
    return (result / (wide * block_len)).reshape(leading + (out_count * block_len,))


def short_filter(padded, filter_taps):
    return (
        padded[..., :-2] * filter_taps[:, 0, :, None]
        + padded[..., 1:-1] * filter_taps[:, 1, :, None]
        + padded[..., 2:] * filter_taps[:, 2, :, None]
    )


def filter_bank(seq_len, filter_in, filter_mid, out_block, rate_block):
    positions = jnp.arange(seq_len, dtype=jnp.float32)
    relative = positions / (seq_len - 1)
    bands = jnp.linspace(0.0001, BANDS - 1, BANDS, dtype=jnp.float32)
    angles = 2 * math.pi / seq_len * positions[:, None] * bands[None, :]
    feats = jnp.concatenate([relative[:, None], jnp.cos(angles), jnp.sin(angles)], axis=1)
    hidden = jnp.sin(jnp.dot(feats, filter_in, precision=HIGHEST))
    hidden = jnp.sin(jnp.dot(hidden, filter_mid, precision=HIGHEST))
    filter_taps = jnp.einsum("lh,hodc->odcl", hidden, out_block, precision=HIGHEST)
    decay = jnp.exp(-relative[None, :] * rate_block[:, None])
    return filter_taps * decay


def on_device(
    tokens,
    w_value,
    w_gate_one,
    w_gate_two,
    short_taps,
    filter_in,
    filter_mid,
    filter_out,
    decay_rate,
    skip,
    w_out,
):
    n_rows = lax.axis_size("row")
    row_index = lax.axis_index("row")
    col_index = lax.axis_index("col")
    local_width = w_value.shape[0]
    chan_dev = local_width // n_rows
    projected = jnp.stack(
        [
            jnp.einsum("td,cd->ct", tokens, weight, preferred_element_type=jnp.float32)
            for weight in (w_value, w_gate_one, w_gate_two)
        ]
    ).astype(jnp.bfloat16)
    block_len = projected.shape[2]
    seq_len = n_rows * block_len
    wide = 2 * n_rows
    moved = lax.all_to_all(projected, "row", split_axis=1, concat_axis=2, tiled=True)
    own_taps = lax.dynamic_slice_in_dim(short_taps, row_index * chan_dev, chan_dev, 2)
    bordered = jnp.pad(moved.astype(jnp.float32), ((0, 0), (0, 0), (1, 1)))
    channel_major = short_filter(bordered, own_taps)
    global_start = col_index * local_width + row_index * chan_dev
    own_out = lax.dynamic_slice_in_dim(filter_out, global_start, chan_dev, 3)
    own_rate = lax.dynamic_slice_in_dim(decay_rate, row_index * chan_dev, chan_dev, 0)
    own_skip = lax.dynamic_slice_in_dim(skip, row_index * chan_dev, chan_dev, 1)
    filter_taps = filter_bank(seq_len, filter_in, filter_mid, own_out, own_rate)
    forward_part = filter_taps[:, 0]
    backward_part = filter_taps[:, 1]
    kern = jnp.concatenate(
        [
            forward_part,
            jnp.zeros(forward_part[..., :1].shape, jnp.float32),
            backward_part[..., 1:][..., ::-1],
        ],
        axis=-1,
    )
    kern_real, kern_imag = forward_transform(kern, wide, wide, block_len)
    signal = channel_major[0]
    for order_index in range(2):
        sig_real, sig_imag = forward_transform(signal, n_rows, wide, block_len)
        prod_real = sig_real * kern_real[order_index] - sig_imag * kern_imag[order_index]
        prod_imag = sig_real * kern_imag[order_index] + sig_imag * kern_real[order_index]
        long_part = inverse_transform(prod_real, prod_imag, n_rows, wide, block_len)
        signal = channel_major[order_index + 1] * (
            long_part + own_skip[order_index][:, None] * signal
        )
    mixer_channels = signal.astype(jnp.bfloat16)
    position_major = lax.all_to_all(mixer_channels, "row", split_axis=1, concat_axis=0, tiled=True)
    totals = jnp.einsum(
        "ct,cd->td",
        lax.all_gather(position_major, "col", axis=0, tiled=True),
        w_out,
        preferred_element_type=jnp.float32,
    )
    return totals.astype(jnp.bfloat16)


STEP = 32


def position_features(seq_len):
    positions = np.arange(seq_len, dtype=np.float32)
    relative = positions / np.float32(seq_len - 1)
    bands = np.linspace(0.0001, BANDS - 1, BANDS, dtype=np.float32)
    angles = np.float32(2 * math.pi / seq_len) * positions[None, :] * bands[:, None]
    return np.concatenate([relative[None, :], np.cos(angles), np.sin(angles)], axis=0)


def table_seeds(seq_len):
    odd = 2 * np.arange(seq_len)[None, :] + 1
    coarse = (STEP * np.arange(seq_len // STEP)[:, None] * odd) % (4 * seq_len)
    fine = (np.arange(STEP)[:, None] * odd) % (4 * seq_len)
    unit = math.pi / (2 * seq_len)
    return (
        np.stack([np.cos(coarse * unit), np.sin(coarse * unit)]).astype(np.float32),
        np.stack([np.cos(fine * unit), np.sin(fine * unit)]).astype(np.float32),
    )


def split_dot(left, table, table_dim):
    high = left.astype(jnp.bfloat16)
    low = (left - high.astype(jnp.float32)).astype(jnp.bfloat16)
    both = jnp.concatenate([high, low], axis=0)
    product = lax.dot_general(
        both, table, (((1,), (table_dim,)), ((), ())), preferred_element_type=jnp.float32
    )
    return product[: left.shape[0]] + product[left.shape[0] :]


def exact_dot(left, right, left_dim):
    return lax.dot_general(
        left,
        right,
        (((left_dim,), (0,)), ((), ())),
        precision=HIGHEST,
        preferred_element_type=jnp.float32,
    )


def make_tables(coarse_ref, fine_ref, cos_ref, sin_ref):
    def fill(index, carry):
        cos_a = coarse_ref[0, pl.ds(index, 1), :]
        sin_a = coarse_ref[1, pl.ds(index, 1), :]
        cos_b = fine_ref[0]
        sin_b = fine_ref[1]
        rows = pl.ds(pl.multiple_of(index * STEP, STEP), STEP)
        cos_ref[rows, :] = (cos_a * cos_b - sin_a * sin_b).astype(jnp.bfloat16)
        sin_ref[rows, :] = (sin_a * cos_b + cos_a * sin_b).astype(jnp.bfloat16)
        return carry

    lax.fori_loop(0, cos_ref.shape[0] // STEP, fill, 0)


def own_column(vector, chan_dev):
    width = vector.shape[1]
    lanes = lax.broadcasted_iota(jnp.int32, (chan_dev, width), 1)
    wanted = lax.broadcasted_iota(jnp.int32, (chan_dev, width), 0) + lax.axis_index("row") * chan_dev
    return jnp.sum(jnp.where(lanes == wanted, vector, 0.0), axis=1, keepdims=True)


def window_tile(chan_dev, total_width):
    start = (lax.axis_index("col") * lax.axis_size("row") + lax.axis_index("row")) * chan_dev
    tile = start // 128
    return tile - tile // (total_width // 128 - 1), start


def window_picks(chan_dev, total_width, window):
    tile, start = window_tile(chan_dev, total_width)
    lanes = lax.broadcasted_iota(jnp.int32, (chan_dev, window), 1)
    wanted = lax.broadcasted_iota(jnp.int32, (chan_dev, window), 0) + (start - tile * 128)
    return jnp.where(lanes == wanted, 1.0, 0.0)


def kernel_spectra(chan_dev, total_width, in_ref, mid_ref, out_ref, rate_ref, feats_ref, cos_ref, sin_ref):
    hidden = jnp.sin(exact_dot(in_ref[...], feats_ref[...], 0))
    hidden = jnp.sin(exact_dot(mid_ref[...], hidden, 0))
    decay = jnp.exp(-feats_ref[0:1, :] * own_column(rate_ref[...], chan_dev))
    not_first = lax.broadcasted_iota(jnp.int32, decay.shape, 1) > 0
    sums, differences = [], []
    picks = window_picks(chan_dev, total_width, out_ref.shape[3])
    for order in range(2):
        own = [
            lax.dot_general(
                picks,
                out_ref[:, order, direction, :],
                (((1,), (1,)), ((), ())),
                precision=HIGHEST,
                preferred_element_type=jnp.float32,
            )
            for direction in range(2)
        ]
        ahead = exact_dot(own[0], hidden, 1) * decay
        behind = jnp.where(not_first, exact_dot(own[1], hidden, 1) * decay, 0.0)
        sums.append(ahead + behind)
        differences.append(ahead - behind)
    scale = 1.0 / cos_ref.shape[0]
    kern_cos = split_dot(jnp.concatenate(sums, axis=0), cos_ref[...], 0) * scale
    kern_sin = split_dot(jnp.concatenate(differences, axis=0), sin_ref[...], 0) * scale
    return kern_cos, kern_sin


def short_rows(blocks, short_ref, which, chan_dev):
    joined = jnp.concatenate([block.astype(jnp.float32) for block in blocks], axis=1)
    length = joined.shape[1]
    lanes = lax.broadcasted_iota(jnp.int32, joined.shape, 1)
    before = jnp.where(lanes == 0, 0.0, pltpu.roll(joined, 1, 1))
    after = jnp.where(lanes == length - 1, 0.0, pltpu.roll(joined, length - 1, 1))
    tap = [own_column(short_ref[which, j : j + 1, :], chan_dev) for j in range(3)]
    return before * tap[0] + joined * tap[1] + after * tap[2]


def long_convolutions(signal_of, spectra, skip_ref, cos_ref, sin_ref, chan_dev):
    kern_cos, kern_sin = spectra
    signal = signal_of(0)
    for order in range(2):
        rows = slice(order * chan_dev, (order + 1) * chan_dev)
        k_cos, k_sin = kern_cos[rows], kern_sin[rows]
        z_cos = split_dot(signal, cos_ref[...], 0)
        z_sin = split_dot(signal, sin_ref[...], 0)
        long_part = split_dot(z_cos * k_cos - z_sin * k_sin, cos_ref[...], 1) + split_dot(
            z_cos * k_sin + z_sin * k_cos, sin_ref[...], 1
        )
        weight = own_column(skip_ref[order : order + 1, :], chan_dev)
        signal = signal_of(order + 1) * (long_part + weight * signal)
    return signal


def flipped(index, mask):
    for bit in range(mask.bit_length()):
        if mask >> bit & 1:
            index = index + (1 - 2 * (index // 2**bit % 2)) * 2**bit
    return index


def mix_kernel(
    n_rows,
    n_cols,
    chan_dev,
    total_width,
    sources,
    result_ref,
    held,
    cos_ref,
    sin_ref,
    projected_ref,
    moved_ref,
    y_ref,
    gathered,
    load_sem,
    weight_sem,
    there_send,
    there_recv,
    back_send,
    back_recv,
    far_send,
    far_recv,
    mate_send,
    mate_recv,
):
    row = lax.axis_index("row")
    col = lax.axis_index("col")
    block_len = moved_ref.shape[3]
    half = n_cols // 2
    mate = col + 1 - 2 * (col % 2)
    gathered_ref = result_ref if gathered is None else gathered
    tile, _ = window_tile(chan_dev, total_width)
    lanes = pl.ds(pl.multiple_of(tile * 128, 128), held["filter_out"].shape[3])
    loads = {}
    pairs = list(range(1, n_rows // 2))[::-1]
    pairs = [p for p in pairs if p >= n_rows // 4] + [p for p in pairs if p < n_rows // 4] + [0]
    pair_rows = 2 * chan_dev

    def load(*names):
        for name in names:
            source = sources[name]
            if name == "filter_out":
                source = source.at[:, :, :, lanes]
            index = list(sources).index(name)
            loads[name] = pltpu.make_async_copy(source, held[name], load_sem.at[index])
            loads[name].start()

    def weight_rows(pair):
        return pl.ds(pl.multiple_of(flipped(row // 2, pair) * pair_rows, pair_rows), pair_rows)

    def load_weight(which, name):
        for pair in pairs:
            rows = weight_rows(pair)
            loads[which, pair] = pltpu.make_async_copy(
                sources[name].at[rows, :], held[name].at[rows, :], weight_sem.at[which, pair]
            )
            loads[which, pair].start()

    load("coarse", "fine", "tokens")
    load_weight(0, "w_value")

    def copy(source, target, send_sem, recv_sem, to_row, to_col):
        return pltpu.make_async_remote_copy(
            src_ref=source,
            dst_ref=target,
            send_sem=send_sem,
            recv_sem=recv_sem,
            device_id=(to_row, to_col),
            device_id_type=pl.DeviceIdType.MESH,
        )

    def row_at(mask):
        return flipped(row, mask)

    def far_at(offset):
        return (col + 2 * offset) % n_cols

    partners = [(row_at(d), col) for d in range(1, n_rows)]
    partners += [(row, far_at(h)) for h in range(1, half)] + [(row, mate)]
    barrier = pltpu.get_barrier_semaphore()
    for partner in partners:
        pl.semaphore_signal(barrier, inc=1, device_id=partner, device_id_type=pl.DeviceIdType.MESH)
    for name in ("coarse", "fine"):
        loads[name].wait()
    make_tables(held["coarse"], held["fine"], cos_ref, sin_ref)
    load_weight(1, "w_first")
    load("filter_in", "filter_mid", "filter_out", "rate", "feats", "short_taps", "skip")
    loads["tokens"].wait()

    there = {}
    for which, name in enumerate(("w_value", "w_first", "w_second")):
        for pair in pairs:
            loads[which, pair].wait()
            product = lax.dot_general(
                held[name][weight_rows(pair), :],
                held["tokens"][...],
                (((1,), (1,)), ((), ())),
                preferred_element_type=jnp.float32,
            )
            for s in range(2):
                target = flipped(row // 2, pair) * 2 + s
                projected_ref[which, target] = product[s * chan_dev : (s + 1) * chan_dev].astype(
                    jnp.bfloat16
                )
            if which == 0 and pair == pairs[0]:
                pl.semaphore_wait(barrier, len(partners))
            for d in (2 * pair, 2 * pair + 1):
                if d == 0:
                    moved_ref[which, row] = projected_ref[which, row]
                    continue
                there[which, d] = copy(
                    projected_ref.at[which, row_at(d)],
                    moved_ref.at[which, row],
                    there_send.at[which, d - 1],
                    there_recv.at[which, d - 1],
                    row_at(d),
                    col,
                )
                there[which, d].start()
        if which == 0:
            load_weight(2, "w_second")
        if which == 1:
            load("w_out")

    for name in ("filter_in", "filter_mid", "filter_out", "rate", "feats", "short_taps", "skip"):
        loads[name].wait()
    spectra = kernel_spectra(
        chan_dev,
        total_width,
        held["filter_in"],
        held["filter_mid"],
        held["filter_out"],
        held["rate"],
        held["feats"],
        cos_ref,
        sin_ref,
    )

    def signal_of(which):
        for d in range(1, n_rows):
            there[which, d].wait_recv()
        return short_rows(
            [moved_ref[which, s] for s in range(n_rows)], held["short_taps"], which, chan_dev
        )

    signal = long_convolutions(signal_of, spectra, held["skip"], cos_ref, sin_ref, chan_dev)
    for s in range(n_rows):
        y_ref[s] = signal[:, s * block_len : (s + 1) * block_len].astype(jnp.bfloat16)
    gathered_ref[col, row] = y_ref[row]

    back = {}
    far_first = [2 * pair + x for pair in pairs for x in range(2) if pair or x]
    for d in far_first:
        back[d] = copy(
            y_ref.at[row_at(d)],
            gathered_ref.at[col, row],
            back_send.at[d - 1],
            back_recv.at[d - 1],
            row_at(d),
            col,
        )
        back[d].start()
    far, near = {}, {}

    def to_mate(h, d):
        block = gathered_ref.at[far_at(h), row_at(d)]
        near[h, d] = copy(block, block, mate_send.at[h, d], mate_recv.at[h, d], row, mate)
        near[h, d].start()

    near_first = [0] + far_first[::-1]
    for d in near_first:
        if d:
            back[d].wait_recv()
        block = gathered_ref.at[col, row_at(d)]
        for h in range(1, half):
            far[h, d] = copy(
                block, block, far_send.at[h - 1, d], far_recv.at[h - 1, d], row, far_at(h)
            )
            far[h, d].start()
        to_mate(0, d)
    group = n_rows * chan_dev

    def add_group(owner, total):
        left = jnp.concatenate(
            [gathered_ref[owner, s].astype(jnp.float32) for s in range(n_rows)], axis=0
        ).astype(jnp.bfloat16)
        rows = pl.ds(pl.multiple_of(owner * group, group), group)
        product = lax.dot_general(
            left,
            held["w_out"][rows, :],
            (((0,), (0,)), ((), ())),
            preferred_element_type=jnp.float32,
        )
        return product if total is None else total + product

    loads["w_out"].wait()
    total = add_group(col, None)
    for h in range(1, half):
        for d in near_first:
            far[h, d].wait_recv()
            to_mate(half - h, d)
    for h in range(half):
        if h:
            total = add_group(far_at(h), total)
        for d in range(n_rows):
            near[h, d].wait_recv()
        total = add_group((mate + 2 * h) % n_cols, total)
    result_ref[...] = total.astype(jnp.bfloat16)
    for send in (there, back, far, near):
        for one in send.values():
            one.wait_send()


def on_device_dense(
    tokens,
    w_value,
    w_gate_one,
    w_gate_two,
    short_taps,
    filter_in,
    filter_mid,
    filter_out,
    decay_rate,
    skip,
    w_out,
):
    n_rows = lax.axis_size("row")
    n_cols = lax.axis_size("col")
    half = n_cols // 2
    local_width = w_value.shape[0]
    chan_dev = local_width // n_rows
    total_width = filter_out.shape[3]
    block_len = tokens.shape[0]
    seq_len = n_rows * block_len
    coarse, fine = table_seeds(seq_len)
    sources = dict(
        tokens=tokens,
        coarse=coarse,
        fine=fine,
        w_value=w_value,
        w_first=w_gate_one,
        w_second=w_gate_two,
        filter_out=filter_out,
        filter_in=filter_in,
        filter_mid=filter_mid,
        rate=decay_rate.reshape(1, local_width),
        feats=position_features(seq_len),
        short_taps=short_taps,
        skip=skip,
        w_out=w_out,
    )
    window = -(-(chan_dev + 127) // 128) * 128
    held = {name: pltpu.VMEM(source.shape, source.dtype) for name, source in sources.items()}
    held["filter_out"] = pltpu.VMEM(filter_out.shape[:3] + (window,), filter_out.dtype)
    dma = pltpu.SemaphoreType.DMA
    collected = (n_cols, n_rows, chan_dev, block_len)
    result = jax.ShapeDtypeStruct((block_len, w_out.shape[1]), jnp.bfloat16)
    gathered = pltpu.VMEM(collected, jnp.bfloat16)
    return_value = pl.pallas_call(
        functools.partial(mix_kernel, n_rows, n_cols, chan_dev, total_width),
        out_shape=result,
        in_specs=[{name: pl.BlockSpec(memory_space=pl.ANY) for name in sources}],
        out_specs=pl.BlockSpec(memory_space=pltpu.VMEM),
        scratch_shapes=[
            held,
            pltpu.VMEM((seq_len, seq_len), jnp.bfloat16),
            pltpu.VMEM((seq_len, seq_len), jnp.bfloat16),
            pltpu.VMEM((3, n_rows, chan_dev, block_len), jnp.bfloat16),
            pltpu.VMEM((3, n_rows, chan_dev, block_len), jnp.bfloat16),
            pltpu.VMEM((n_rows, chan_dev, block_len), jnp.bfloat16),
            gathered,
            dma((len(sources),)),
            dma((3, n_rows // 2)),
            dma((3, n_rows - 1)),
            dma((3, n_rows - 1)),
            dma((n_rows - 1,)),
            dma((n_rows - 1,)),
            dma((half - 1, n_rows)),
            dma((half - 1, n_rows)),
            dma((half, n_rows)),
            dma((half, n_rows)),
        ],
        compiler_params=pltpu.CompilerParams(
            vmem_limit_bytes=56 << 20, collective_id=0, has_side_effects=True
        ),
    )(sources)
    return return_value


def solution(mesh):
    placed = (
        P("row", None),
        P("col", None),
        P("col", None),
        P("col", None),
        P(None, None, "col"),
        P(),
        P(),
        P(),
        P("col"),
        P(None, "col"),
        P(None, "col"),
    )

    def program(tokens, w_value, *rest):
        seq_len = tokens.shape[0]
        devices = mesh.shape["row"] * mesh.shape["col"]
        columns = mesh.shape["col"]
        dense = (
            seq_len <= 2048
            and seq_len // mesh.shape["row"] % 128 == 0
            and w_value.shape[0] // devices % 8 == 0
            and columns % 2 == 0
            and columns > 2
            and mesh.shape["row"] >= 4
            and mesh.shape["row"] & (mesh.shape["row"] - 1) == 0
            and rest[5].shape[3] % 128 == 0
            and w_value.shape[0] // devices <= 129
            and rest[5].shape[3] >= 384
        )
        body = on_device_dense if dense else on_device
        return jax.shard_map(
            body, mesh=mesh, in_specs=placed, out_specs=P("row", "col"), check_vma=False
        )(tokens, w_value, *rest)

    return program
```
